32 devices in a mesh: sp: 8 (over z, y), tp: 4 (over x, core).
Axes of the slice: x: 2, y: 2, z: 4, core: 2. Of those that a mesh axis runs over, the one named last changes fastest.
Arguments:
- stream: bfloat16 [8192, 2048], P(('sp', 'tp')), may hold values from -6 to 6
- query_rows: bfloat16 [8192, 1024], P('sp', 'tp'), may hold values from -6 to 6
- key_rows: bfloat16 [8192, 1024], P('sp', 'tp'), may hold values from -6 to 6
- value_rows: bfloat16 [8192, 2048], P('sp', 'tp'), may hold values from -6 to 6
- gate_rows: bfloat16 [8192, 2048], P('sp', 'tp'), may hold values from -6 to 6
- log_decay: float32 [8192, 1024], P('sp', 'tp'), may hold values from -1 to 0
- head_gain: float32 [256], replicated, may hold values from 0.1 to 1.9
- out_weight: bfloat16 [2048, 2048], P('tp'), may hold values from -0.125 to 0.125
- mix_gain: float32 [2048], replicated, may hold values from 0.1 to 1.9
- up_weight: bfloat16 [2048, 8192], P('sp', 'tp'), may hold values from -0.125 to 0.125
- down_weight: bfloat16 [2048, 8192], P('sp', 'tp'), may hold values from -0.0625 to 0.0625
Outputs:
- mixed_out: bfloat16 [8192, 2048], P(('sp', 'tp'))
The draws below stay inside these ranges and needn't reach their ends.
All inputs are finite; a program needn't handle non-finite values.
Results may differ from the reference program's by a relative error of at most 0.02.
Values may be sent and summed in bfloat16 or wider, within the bound.
A program may use at most 128 MiB of HBM per device.

```python
import jax
import jax.numpy as jnp
from jax import lax

D = 2048
HEADS = 8
KEY_CHANNELS = 128
DV = 256
FF = 8192
BLOCK = 64
TOK_DEV = 1024
TOKENS = 8192
N_TP = 4


def draw_log_decay(key, part):
    keys = jax.random.split(jax.random.fold_in(key, 7), 7)
    devices = TOKENS // TOK_DEV
    width = HEADS * KEY_CHANNELS
    fast_share = 0.5
    noise = jax.random.uniform(keys[4], (TOKENS, width), jnp.float32, 0.5, 1.5)
    fast_head = jax.random.uniform(keys[0], (HEADS,), jnp.float32) < fast_share
    fast_channel = jnp.repeat(fast_head, KEY_CHANNELS)
    slow_rate = jnp.exp(jax.random.uniform(keys[1], (width,), jnp.float32, jnp.log(0.1), jnp.log(0.5))) / TOKENS
    fast_rate = jnp.exp(jax.random.uniform(keys[2], (width,), jnp.float32, jnp.log(0.02), jnp.log(0.033)))
    base = jnp.where(fast_channel, fast_rate, slow_rate)
    device_factor = jnp.exp(jax.random.uniform(keys[3], (devices, HEADS), jnp.float32, jnp.log(0.5), jnp.log(2.0)))
    device_rows = jnp.repeat(jnp.repeat(device_factor, TOK_DEV, axis=0), KEY_CHANNELS, axis=1)
    decay_rates = base[None, :] * device_rows * noise
    spots = jax.random.randint(keys[5], (2,), 0, TOKENS)
    decay_losses = jax.random.uniform(keys[6], (2, HEADS), jnp.float32, 0.2, 0.4)
    block_hits = (jnp.arange(TOKENS)[:, None] == spots[None, :]).astype(jnp.float32)
    block_surge = jnp.dot(block_hits, jnp.log(1.0 - decay_losses))
    return (jnp.repeat(block_surge, KEY_CHANNELS, axis=1) - decay_rates).astype(jnp.float32)


def shard_levels(own_key, shape, shards, smallest, largest):
    level = 1.0
    for dim, blocks in shards:
        steps = jax.random.uniform(jax.random.fold_in(jax.random.fold_in(own_key, 6), dim), (blocks,), jnp.float32, smallest / len(shards), largest / len(shards))
        level = level * jnp.repeat(jnp.exp(steps), shape[dim] // blocks).reshape((-1,) + (1,) * (len(shape) - 1 - dim))
    return level


def centred(rng, extent, scale, most, pieces=(), held_as=jnp.bfloat16):
    result = scale * jax.random.normal(rng, extent, jnp.float32)
    if pieces:
        result = result * shard_levels(rng, extent, pieces, -0.22, 0.18)
    return jnp.clip(result, -most, most).astype(held_as)


def setup_inputs(seed: int = 0) -> dict:
    key_of = jax.random.split(jax.random.key(seed), 12)
    stream = centred(key_of[0], (TOKENS, D), 1.0, 6.0, ((0, 32),))
    query_rows = centred(key_of[1], (TOKENS, HEADS * KEY_CHANNELS), 1.0, 6.0, ((0, 8), (1, 4)))
    key_rows = centred(key_of[2], (TOKENS, HEADS * KEY_CHANNELS), 1.0, 6.0, ((0, 8), (1, 4)))
    value_rows = centred(key_of[3], (TOKENS, HEADS * DV), 1.0, 6.0, ((0, 8), (1, 4)))
    gate_rows = centred(key_of[4], (TOKENS, HEADS * DV), 1.0, 6.0, ((0, 8), (1, 4)))
    log_decay = draw_log_decay(jax.random.fold_in(key_of[11], 71), 0)
    head_gain = jnp.clip(1.0 + 0.18 * jax.random.normal(key_of[6], (DV,), jnp.float32), 0.1, 1.9)
    out_weight = centred(key_of[7], (HEADS * DV, D), (HEADS * DV) ** -0.5, 0.125, ((0, 4),))
    mix_gain = jnp.clip(1.0 + 0.18 * jax.random.normal(key_of[8], (D,), jnp.float32), 0.1, 1.9)
    up_weight = centred(key_of[9], (D, FF), D ** -0.5, 0.125, ((0, 8), (1, 4)))
    down_weight = centred(key_of[10], (D, FF), FF ** -0.5, 0.0625, ((0, 8), (1, 4)))
    return {"stream": stream, "query_rows": query_rows, "key_rows": key_rows, "value_rows": value_rows, "gate_rows": gate_rows, "log_decay": log_decay, "head_gain": head_gain, "out_weight": out_weight, "mix_gain": mix_gain, "up_weight": up_weight, "down_weight": down_weight}


EPS = 1e-06

def attention(query_rows, key_rows, value_rows, log_decay):
    count = TOKENS // BLOCK
    queries = query_rows.astype(jnp.float32).reshape(count, BLOCK, HEADS, KEY_CHANNELS) * KEY_CHANNELS ** (-0.5)
    keys_all = key_rows.astype(jnp.float32).reshape(count, BLOCK, HEADS, KEY_CHANNELS)
    values_all = value_rows.astype(jnp.float32).reshape(count, BLOCK, HEADS, DV)
    decay_rates = log_decay.astype(jnp.float32).reshape(count, BLOCK, HEADS, KEY_CHANNELS)

    def step(matrix_state, inputs):
        query_block, kee, value_block, rate = inputs
        cum = jnp.cumsum(rate, axis=0)
        last = cum[-1:]
        decayed_state = kee * jnp.exp(last - cum)
        state_update = jnp.einsum('qzx,qzf->zxf', decayed_state, value_block, precision=lax.Precision.HIGHEST)
        matrix_state = jnp.exp(last[0])[..., None] * matrix_state + state_update
        head_output = jnp.einsum('wle,leg->wlg', query_block, matrix_state, precision=lax.Precision.HIGHEST)
        return (matrix_state, head_output)
    start = jnp.zeros((HEADS, KEY_CHANNELS, DV), jnp.float32)
    _, outs = lax.scan(step, start, (queries, keys_all, values_all, decay_rates))
    return outs.reshape(TOKENS, HEADS, DV)

def feed_block(rows_in, up_weight, down_weight):
    pre = jnp.dot(rows_in, up_weight, preferred_element_type=jnp.float32)
    hidden = jnp.square(jax.nn.relu(pre)).astype(jnp.bfloat16)
    group = FF // N_TP
    grouped = hidden.astype(jnp.float32).reshape(rows_in.shape[0], N_TP, group)
    downs = down_weight.astype(jnp.float32).reshape(D, N_TP, group)
    parts = jnp.einsum('rjf,djf->jrd', grouped, downs)
    parts = lax.optimization_barrier(parts.astype(jnp.bfloat16)).astype(jnp.float32)
    return lax.optimization_barrier(jnp.sum(parts, axis=0))

def reference(stream, query_rows, key_rows, value_rows, gate_rows, log_decay, head_gain, out_weight, mix_gain, up_weight, down_weight):
    readout = attention(query_rows, key_rows, value_rows, log_decay)
    scaled = readout * lax.rsqrt(lax.optimization_barrier(jnp.mean(readout * readout, axis=-1, keepdims=True)) + EPS)
    gates = gate_rows.astype(jnp.float32).reshape(TOKENS, HEADS, DV)
    gated = scaled * head_gain.astype(jnp.float32) * jax.nn.silu(gates)
    heads_out = gated.reshape(TOKENS, HEADS * DV).astype(jnp.bfloat16)
    attn = jnp.dot(heads_out, out_weight, preferred_element_type=jnp.float32)
    mid = (stream.astype(jnp.float32) + attn).astype(jnp.bfloat16)
    midf = mid.astype(jnp.float32)
    normed = (midf * lax.rsqrt(lax.optimization_barrier(jnp.mean(midf * midf, axis=-1, keepdims=True)) + EPS) * mix_gain.astype(jnp.float32)).astype(jnp.bfloat16)
    blocks = normed.reshape(TOKENS // TOK_DEV, TOK_DEV, D)
    feed = lax.map(lambda rows_in: feed_block(rows_in, up_weight, down_weight), blocks).reshape(TOKENS, D)
    return (midf + feed).astype(jnp.bfloat16)
```

```python
import functools

import jax
import jax.numpy as jnp
from jax import lax
from jax.experimental import pallas as pl
from jax.experimental.pallas import tpu as pltpu
from jax.sharding import PartitionSpec as P

KEY_CHANNELS = 128
DV = 256
BLOCK = 64
EPS = 1e-06


NT = (((1,), (1,)), ((), ()))
TN = (((0,), (0,)), ((), ()))


def local_states(q_ref, k_ref, v_ref, ld_ref, out_ref, qd_ref, state_ref):
    count = q_ref.shape[0] // BLOCK
    row = lax.broadcasted_iota(jnp.int32, (BLOCK, BLOCK), 0)
    col = lax.broadcasted_iota(jnp.int32, (BLOCK, BLOCK), 1)
    later = (col > row).astype(jnp.float32)
    scale = KEY_CHANNELS ** (-0.5)
    state = jnp.zeros((DV, KEY_CHANNELS), jnp.float32)
    total = jnp.zeros((1, KEY_CHANNELS), jnp.float32)
    for c in range(count):
        rows = pl.ds(c * BLOCK, BLOCK)
        rates = ld_ref[rows, :]
        rest = jnp.dot(later, rates, precision=lax.Precision.HIGHEST, preferred_element_type=jnp.float32)
        last = jnp.sum(rates, axis=0, keepdims=True)
        keys = (k_ref[rows, :].astype(jnp.float32) * jnp.exp(rest)).astype(jnp.bfloat16)
        update = lax.dot_general(v_ref[rows, :], keys, TN, preferred_element_type=jnp.float32)
        state = state * jnp.exp(last) + update
        total = total + last
        q = q_ref[rows, :]
        out_ref[rows, :] = lax.dot_general(
            q, state.astype(jnp.bfloat16), NT, preferred_element_type=jnp.float32
        ) * scale
        qd_ref[rows, :] = (q.astype(jnp.float32) * (jnp.exp(total) * scale)).astype(jnp.bfloat16)
    state_ref[0, :DV, :] = state.astype(jnp.bfloat16)
    state_ref[0, DV:, :] = jnp.broadcast_to(jnp.exp(total), (16, KEY_CHANNELS)).astype(jnp.bfloat16)


def finish_heads(own_ref, qd_ref, state_ref, gate_ref, gain_ref, out_ref):
    readout = own_ref[...] + lax.dot_general(
        qd_ref[...], state_ref[0, :DV, :], NT, preferred_element_type=jnp.float32
    )
    scaled = readout * lax.rsqrt(jnp.mean(readout * readout, axis=-1, keepdims=True) + EPS)
    gates = gate_ref[...].astype(jnp.float32)
    out_ref[...] = (scaled * gain_ref[...] * (gates / (1.0 + jnp.exp(-gates)))).astype(jnp.bfloat16)


def attention_local(q, k, v, ld):
    rows = q.shape[0]
    heads = q.shape[1] // KEY_CHANNELS
    kb = pl.BlockSpec((rows, KEY_CHANNELS), lambda h: (0, h))
    vb = pl.BlockSpec((rows, DV), lambda h: (0, h))
    return pl.pallas_call(
        local_states,
        grid=(heads,),
        in_specs=[kb, kb, vb, kb],
        out_specs=[vb, kb, pl.BlockSpec((1, DV + 16, KEY_CHANNELS), lambda h: (h, 0, 0))],
        out_shape=[
            jax.ShapeDtypeStruct((rows, heads * DV), jnp.float32),
            jax.ShapeDtypeStruct((rows, heads * KEY_CHANNELS), jnp.bfloat16),
            jax.ShapeDtypeStruct((heads, DV + 16, KEY_CHANNELS), jnp.bfloat16),
        ],
        cost_estimate=pl.CostEstimate(flops=6_000_000_000, bytes_accessed=8_000_000, transcendentals=0),
        name="local_states",
    )(q, k, v, ld)


def attention_finish(own, qd, state, gates, gain):
    rows = own.shape[0]
    heads = own.shape[1] // DV
    tile = rows // 2
    vb = pl.BlockSpec((tile, DV), lambda h, r: (r, h))
    return pl.pallas_call(
        finish_heads,
        grid=(heads, rows // tile),
        in_specs=[
            vb,
            pl.BlockSpec((tile, KEY_CHANNELS), lambda h, r: (r, h)),
            pl.BlockSpec((1, DV + 16, KEY_CHANNELS), lambda h, r: (h, 0, 0)),
            vb,
            pl.BlockSpec((1, DV), lambda h, r: (0, 0)),
        ],
        out_specs=vb,
        out_shape=jax.ShapeDtypeStruct(own.shape, jnp.bfloat16),
        cost_estimate=pl.CostEstimate(flops=3_000_000_000, bytes_accessed=4_000_000, transcendentals=0),
        name="finish_heads",
    )(own, qd, state, gates, gain)


def incoming_state(own, n):
    def shifted(a, by):
        return lax.ppermute(a, "sp", [(i, i + by) for i in range(n - by)])

    x = shifted(own, 1)
    by = 1
    while by < n - 1:
        e = shifted(x, by).astype(jnp.float32)
        f = x.astype(jnp.float32)
        decay = f[:, DV : DV + 1]
        x = jnp.concatenate(
            [decay * e[:, :DV] + f[:, :DV], jnp.broadcast_to(decay * e[:, DV : DV + 1], e[:, DV:].shape)], axis=1
        ).astype(jnp.bfloat16)
        by *= 2
    return x


def cycle_of(n):
    return list(range(0, n, 2)) + list(range(n - 1 - n % 2, 0, -2))


class Ring:
    def __init__(self, piece, n):
        self.n, self.cyc, self.piece = n, cycle_of(n), piece
        self.fwd = [(self.cyc[i], self.cyc[(i + 1) % n]) for i in range(n)]
        self.bwd = [(b, a) for a, b in self.fwd]
        self.left = self.right = piece
        self.hops = n // 2

    def hop(self, h):
        left, right = self.left, self.right
        if h == self.hops:
            half = self.piece.shape[0] // 2
            left, right = left[:half], right[half:]
        self.left = lax.ppermute(left, "sp", self.fwd)
        self.right = lax.ppermute(right, "sp", self.bwd)
        if h == self.hops:
            return [jnp.concatenate([self.left, self.right], axis=0)]
        return [self.left, self.right]


def owner_of(n, h):
    cyc = cycle_of(n)
    place = [0] * n
    for i, d in enumerate(cyc):
        place[d] = i
    me = jnp.asarray(place, jnp.int32)[lax.axis_index("sp")]
    cyc = jnp.asarray(cyc, jnp.int32)
    if h == 0:
        return [cyc[me]]
    back = cyc[(me - h) % n]
    return [back] if 2 * h == n else [back, cyc[(me + h) % n]]


def local(
    n_sp, n_tp, stream, query_rows, key_rows, value_rows, gate_rows, log_decay, head_gain, out_weight, mix_gain,
    up_weight, down_weight,
):
    nx = n_tp // 2
    own_rows = stream.shape[0]
    me = lax.axis_index("tp")
    x, core = me // 2, me % 2

    def across(a, dx):
        return lax.ppermute(a, "tp", [(((i // 2 + dx) % nx) * 2 + i % 2, i) for i in range(n_tp)])

    def swap(a):
        return lax.ppermute(a, "tp", [(i ^ 1, i) for i in range(n_tp)])

    up = Ring(up_weight, n_sp)
    down = Ring(down_weight, n_sp)
    width = up_weight.shape[0]
    up_full = lax.dynamic_update_slice_in_dim(
        jnp.zeros((width * n_sp, up_weight.shape[1]), up_weight.dtype), up_weight, owner_of(n_sp, 0)[0] * width, 0
    )

    ups = [up.hop(h) for h in range(1, up.hops + 1)]
    down.left, down.right, _ = lax.optimization_barrier((down.left, down.right, ups[1][0][:8]))
    downs = [[down_weight]] + [down.hop(h) for h in range(1, down.hops + 1)]

    w = {(0, 0): out_weight}
    for dx in range(1, nx):
        w[dx, 0] = across(out_weight, dx)
    for dx in range(nx):
        w[dx, 1] = swap(w[dx, 0])

    own, qd, summary = attention_local(query_rows, key_rows, value_rows, log_decay)
    before = incoming_state(summary, n_sp)
    heads_out = attention_finish(own, qd, before, gate_rows, head_gain.reshape(1, DV))

    attn = None
    for dx in range(nx):
        for dc in range(2):
            to = ((x - dx) % nx) * 2 + (core + dc) % 2
            block = lax.dynamic_slice_in_dim(heads_out, to * own_rows, own_rows, 0)
            if (dx, dc) != (0, 0):
                block = lax.ppermute(
                    block, "tp", [(((i // 2 + dx) % nx) * 2 + (i % 2 + dc) % 2, i) for i in range(n_tp)]
                )
            term = jnp.dot(block, w[dx, dc], preferred_element_type=jnp.float32)
            attn = term if attn is None else attn + term
    midf = (stream.astype(jnp.float32) + attn).astype(jnp.bfloat16).astype(jnp.float32)
    normed = (
        midf * lax.rsqrt(jnp.mean(midf * midf, axis=-1, keepdims=True) + EPS) * mix_gain
    ).astype(jnp.bfloat16)

    for h, pieces in enumerate(ups, 1):
        for piece, who in zip(pieces, owner_of(n_sp, h)):
            up_full = lax.dynamic_update_slice_in_dim(up_full, piece, who * width, 0)

    n = {(0, 0): normed}
    for dx in range(1, nx):
        n[dx, 0] = across(normed, dx)
    for dx in range(nx):
        n[dx, 1] = swap(n[dx, 0])
    order = [(dx, dc) for dc in range(2) for dx in range(nx)]

    def hidden_of(rows):
        pre = jnp.dot(rows, up_full, preferred_element_type=jnp.float32)
        return jnp.square(jax.nn.relu(pre)).astype(jnp.bfloat16)

    hidden = jnp.concatenate([hidden_of(n[key]) for key in order], axis=0)

    out = jnp.zeros(stream.shape, jnp.bfloat16)
    mid = midf.astype(jnp.bfloat16)
    for h, pieces in enumerate(downs):
        whole = jnp.concatenate(pieces, axis=0) if len(pieces) > 1 else pieces[0]
        part = lax.dot_general(hidden, whole, NT, preferred_element_type=jnp.float32).astype(jnp.bfloat16)
        half = nx * own_rows
        both = part[:half].astype(jnp.float32) + swap(part[half:]).astype(jnp.float32)
        feed = both[:own_rows]
        for dx in range(1, nx):
            send = both[dx * own_rows : (dx + 1) * own_rows].astype(jnp.bfloat16)
            feed = feed + across(send, nx - dx).astype(jnp.float32)
        for j, who in enumerate(owner_of(n_sp, h)):
            cols = lax.dynamic_slice_in_dim(mid, who * width, width, 1).astype(jnp.float32)
            done = (cols + feed[:, j * width : (j + 1) * width]).astype(jnp.bfloat16)
            out = lax.dynamic_update_slice_in_dim(out, done, who * width, 1)
    return out


def solution(mesh):
    placed = (
        P(("sp", "tp"), None),
        P("sp", "tp"),
        P("sp", "tp"),
        P("sp", "tp"),
        P("sp", "tp"),
        P("sp", "tp"),
        P(),
        P("tp", None),
        P(),
        P("sp", "tp"),
        P("sp", "tp"),
    )
    body = functools.partial(local, mesh.shape["sp"], mesh.shape["tp"])
    return jax.shard_map(body, mesh=mesh, in_specs=placed, out_specs=P(("sp", "tp"), None), check_vma=False)
```

```python
import jax
import jax.numpy as jnp
from jax import lax
from jax.experimental import pallas as pl
from jax.sharding import PartitionSpec as P


KEY_CHANNELS = 128
DV = 256
BLOCK = 64
EPS = 1e-06


NT = (((1,), (1,)), ((), ()))
TN = (((0,), (0,)), ((), ()))


def local_states(q_ref, k_ref, v_ref, ld_ref, out_ref, qd_ref, state_ref):
    count = q_ref.shape[0] // BLOCK
    row = lax.broadcasted_iota(jnp.int32, (BLOCK, BLOCK), 0)
    col = lax.broadcasted_iota(jnp.int32, (BLOCK, BLOCK), 1)
    later = (col > row).astype(jnp.float32)
    scale = KEY_CHANNELS ** (-0.5)
    state = jnp.zeros((DV, KEY_CHANNELS), jnp.float32)
    total = jnp.zeros((1, KEY_CHANNELS), jnp.float32)
    for c in range(count):
        rows = pl.ds(c * BLOCK, BLOCK)
        rates = ld_ref[rows, :]
        rest = jnp.dot(later, rates, precision=lax.Precision.HIGHEST, preferred_element_type=jnp.float32)
        last = jnp.sum(rates, axis=0, keepdims=True)
        keys = (k_ref[rows, :].astype(jnp.float32) * jnp.exp(rest)).astype(jnp.bfloat16)
        update = lax.dot_general(v_ref[rows, :], keys, TN, preferred_element_type=jnp.float32)
        state = state * jnp.exp(last) + update
        total = total + last
        q = q_ref[rows, :]
        out_ref[rows, :] = lax.dot_general(
            q, state.astype(jnp.bfloat16), NT, preferred_element_type=jnp.float32
        ) * scale
        qd_ref[rows, :] = (q.astype(jnp.float32) * (jnp.exp(total) * scale)).astype(jnp.bfloat16)
    state_ref[0, :DV, :] = state.astype(jnp.bfloat16)
    state_ref[0, DV:, :] = jnp.broadcast_to(jnp.exp(total), (16, KEY_CHANNELS)).astype(jnp.bfloat16)


def finish_heads(own_ref, qd_ref, state_ref, gate_ref, gain_ref, out_ref):
    readout = own_ref[...] + lax.dot_general(
        qd_ref[...], state_ref[0, :DV, :], NT, preferred_element_type=jnp.float32
    )
    scaled = readout * lax.rsqrt(jnp.mean(readout * readout, axis=-1, keepdims=True) + EPS)
    gates = gate_ref[...].astype(jnp.float32)
    out_ref[...] = (scaled * gain_ref[...] * (gates / (1.0 + jnp.exp(-gates)))).astype(jnp.bfloat16)


def attention_local(q, k, v, ld):
    rows = q.shape[0]
    heads = q.shape[1] // KEY_CHANNELS
    kb = pl.BlockSpec((rows, KEY_CHANNELS), lambda h: (0, h))
    vb = pl.BlockSpec((rows, DV), lambda h: (0, h))
    return pl.pallas_call(
        local_states,
        grid=(heads,),
        in_specs=[kb, kb, vb, kb],
        out_specs=[vb, kb, pl.BlockSpec((1, DV + 16, KEY_CHANNELS), lambda h: (h, 0, 0))],
        out_shape=[
            jax.ShapeDtypeStruct((rows, heads * DV), jnp.float32),
            jax.ShapeDtypeStruct((rows, heads * KEY_CHANNELS), jnp.bfloat16),
            jax.ShapeDtypeStruct((heads, DV + 16, KEY_CHANNELS), jnp.bfloat16),
        ],
        cost_estimate=pl.CostEstimate(flops=6_000_000_000, bytes_accessed=8_000_000, transcendentals=0),
        name="local_states",
    )(q, k, v, ld)


def attention_finish(own, qd, state, gates, gain):
    rows = own.shape[0]
    heads = own.shape[1] // DV
    tile = rows // 2
    vb = pl.BlockSpec((tile, DV), lambda h, r: (r, h))
    return pl.pallas_call(
        finish_heads,
        grid=(heads, rows // tile),
        in_specs=[
            vb,
            pl.BlockSpec((tile, KEY_CHANNELS), lambda h, r: (r, h)),
            pl.BlockSpec((1, DV + 16, KEY_CHANNELS), lambda h, r: (h, 0, 0)),
            vb,
            pl.BlockSpec((1, DV), lambda h, r: (0, 0)),
        ],
        out_specs=vb,
        out_shape=jax.ShapeDtypeStruct(own.shape, jnp.bfloat16),
        cost_estimate=pl.CostEstimate(flops=3_000_000_000, bytes_accessed=4_000_000, transcendentals=0),
        name="finish_heads",
    )(own, qd, state, gates, gain)


def join(earlier, later):
    e, f = earlier.astype(jnp.float32), later.astype(jnp.float32)
    decay = f[:, DV : DV + 1]
    return jnp.concatenate(
        [decay * e[:, :DV] + f[:, :DV], jnp.broadcast_to(decay * e[:, DV : DV + 1], e[:, DV:].shape)], axis=1
    ).astype(jnp.bfloat16)


def shifted(a, by, n):
    return lax.ppermute(a, "sp", [(i, i + by) for i in range(n - by)])


def cycle_of(n):
    return list(range(0, n, 2)) + list(range(n - 1 - n % 2, 0, -2))


class Ring:
    def __init__(self, piece, n):
        self.n, self.cyc, self.piece = n, cycle_of(n), piece
        self.fwd = [(self.cyc[i], self.cyc[(i + 1) % n]) for i in range(n)]
        self.bwd = [(b, a) for a, b in self.fwd]
        self.left = self.right = piece
        self.hops = n // 2

    def hop(self, h):
        left, right = self.left, self.right
        if h == self.hops:
            half = self.piece.shape[0] // 2
            left, right = left[:half], right[half:]
        self.left = lax.ppermute(left, "sp", self.fwd)
        self.right = lax.ppermute(right, "sp", self.bwd)
        if h == self.hops:
            return [jnp.concatenate([self.left, self.right], axis=0)]
        return [self.left, self.right]


def owner_of(n, h):
    cyc = cycle_of(n)
    place = [0] * n
    for i, d in enumerate(cyc):
        place[d] = i
    me = jnp.asarray(place, jnp.int32)[lax.axis_index("sp")]
    cyc = jnp.asarray(cyc, jnp.int32)
    if h == 0:
        return [cyc[me]]
    back = cyc[(me - h) % n]
    return [back] if 2 * h == n else [back, cyc[(me + h) % n]]


def local(
    n_sp, n_tp, stream, query_rows, key_rows, value_rows, gate_rows, log_decay, head_gain, out_weight, mix_gain,
    up_weight, down_weight,
):
    nx = n_tp // 2
    own_rows = stream.shape[0]
    me = lax.axis_index("tp")
    x, core = me // 2, me % 2

    def across(a, dx):
        return lax.ppermute(a, "tp", [(((i // 2 + dx) % nx) * 2 + i % 2, i) for i in range(n_tp)])

    def swap(a):
        return lax.ppermute(a, "tp", [(i ^ 1, i) for i in range(n_tp)])

    up = Ring(up_weight, n_sp)
    down = Ring(down_weight, n_sp)
    width = up_weight.shape[0]
    up_full = lax.dynamic_update_slice_in_dim(
        jnp.zeros((width * n_sp, up_weight.shape[1]), up_weight.dtype), up_weight, owner_of(n_sp, 0)[0] * width, 0
    )
    ups = [up.hop(1)]
    downs = [[down_weight]]

    def tie(a, ring):
        a, ring.left, ring.right = lax.optimization_barrier((a, ring.left, ring.right))
        return a

    w = {(0, 0): out_weight}
    for dx in range(1, nx):
        w[dx, 0] = across(out_weight, dx)
    for dx in range(nx):
        w[dx, 1] = swap(w[dx, 0])

    own, qd, summary = attention_local(query_rows, key_rows, value_rows, log_decay)
    before, covered = tie(shifted(summary, 1, n_sp), up), 1
    while covered < n_sp - 1:
        wider = join(before, summary)
        if len(ups) < up.hops - 1:
            ups.append(up.hop(len(ups) + 1))
        before, covered = join(shifted(wider, covered + 1, n_sp), before), 2 * covered + 1
        before = tie(before, up)
    while len(ups) < up.hops:
        ups.append(up.hop(len(ups) + 1))
    before, down.left, down.right = lax.optimization_barrier((before, down.left, down.right))
    downs.append(down.hop(1))
    heads_out = attention_finish(own, qd, before, gate_rows, head_gain.reshape(1, DV))

    attn = None
    for dx in range(nx):
        for dc in range(2):
            to = ((x - dx) % nx) * 2 + (core + dc) % 2
            block = lax.dynamic_slice_in_dim(heads_out, to * own_rows, own_rows, 0)
            if (dx, dc) != (0, 0):
                block = lax.ppermute(
                    block, "tp", [(((i // 2 + dx) % nx) * 2 + (i % 2 + dc) % 2, i) for i in range(n_tp)]
                )
            term = jnp.dot(block, w[dx, dc], preferred_element_type=jnp.float32)
            attn = term if attn is None else attn + term
    midf = (stream.astype(jnp.float32) + attn).astype(jnp.bfloat16).astype(jnp.float32)
    normed = (
        midf * lax.rsqrt(jnp.mean(midf * midf, axis=-1, keepdims=True) + EPS) * mix_gain
    ).astype(jnp.bfloat16)

    normed = tie(normed, down)
    downs.append(down.hop(2))

    for h, pieces in enumerate(ups, 1):
        for piece, who in zip(pieces, owner_of(n_sp, h)):
            up_full = lax.dynamic_update_slice_in_dim(up_full, piece, who * width, 0)

    n = {(0, 0): normed}
    for dx in range(1, nx):
        n[dx, 0] = across(normed, dx)
    for dx in range(nx):
        n[dx, 1] = swap(n[dx, 0])
    n[nx - 1, 1] = tie(n[nx - 1, 1], down)
    while len(downs) <= down.hops:
        downs.append(down.hop(len(downs)))
    order = [(dx, dc) for dc in range(2) for dx in range(nx)]

    def hidden_of(rows):
        pre = jnp.dot(rows, up_full, preferred_element_type=jnp.float32)
        return jnp.square(jax.nn.relu(pre)).astype(jnp.bfloat16)

    hiddens = []
    for key in order:
        hiddens.append(hidden_of(n[key]))
    hidden = jnp.concatenate(hiddens, axis=0)

    out = jnp.zeros(stream.shape, jnp.bfloat16)
    mid = midf.astype(jnp.bfloat16)
    for h, pieces in enumerate(downs):
        whole = jnp.concatenate(pieces, axis=0) if len(pieces) > 1 else pieces[0]
        part = lax.dot_general(hidden, whole, NT, preferred_element_type=jnp.float32).astype(jnp.bfloat16)
        hidden, part = lax.optimization_barrier((hidden, part))
        half = nx * own_rows
        both = part[:half].astype(jnp.float32) + swap(part[half:]).astype(jnp.float32)
        feed = both[:own_rows]
        for dx in range(1, nx):
            send = both[dx * own_rows : (dx + 1) * own_rows].astype(jnp.bfloat16)
            feed = feed + across(send, nx - dx).astype(jnp.float32)
        for j, who in enumerate(owner_of(n_sp, h)):
            cols = lax.dynamic_slice_in_dim(mid, who * width, width, 1).astype(jnp.float32)
            done = (cols + feed[:, j * width : (j + 1) * width]).astype(jnp.bfloat16)
            out = lax.dynamic_update_slice_in_dim(out, done, who * width, 1)
    return out


def solution(mesh):
    placed = (
        P(("sp", "tp"), None),
        P("sp", "tp"),
        P("sp", "tp"),
        P("sp", "tp"),
        P("sp", "tp"),
        P("sp", "tp"),
        P(),
        P("tp", None),
        P(),
        P("sp", "tp"),
        P("sp", "tp"),
    )

    def body(*args):
        return local(mesh.shape["sp"], mesh.shape["tp"], *args)

    return jax.shard_map(body, mesh=mesh, in_specs=placed, out_specs=P(("sp", "tp"), None), check_vma=False)
```
